32 devices in a mesh: sp: 8 (over z, x), tp: 4 (over y, core).
Axes of the slice: x: 2, y: 2, z: 4, core: 2. Of those that a mesh axis runs over, the one named last changes fastest.
Arguments:
- tokens: bfloat16 [6144, 2048], P(('sp', 'tp')), may hold values from -6 to 6
- in_gain: float32 [2048], replicated, may hold values from 0.1 to 1.9
- w_query: bfloat16 [2048, 1024], P(None, 'tp'), may hold values from -0.125 to 0.125
- w_key: bfloat16 [2048, 1024], P(None, 'tp'), may hold values from -0.125 to 0.125
- w_value: bfloat16 [2048, 2048], P(None, 'tp'), may hold values from -0.125 to 0.125
- w_input_gate: bfloat16 [2048, 8], replicated, may hold values from -8 to 8
- w_forget_gate: bfloat16 [2048, 8], replicated, may hold values from -0.125 to 0.125
- forget_bias: float32 [8], replicated
- forget_extra: float32 [6144, 8], P('sp', 'tp'), may hold values from -2 to 0
- w_conv_gate: bfloat16 [2048, 2048], P(None, 'tp'), may hold values from -0.125 to 0.125
- w_conv_left: bfloat16 [2048, 2048], P(None, 'tp'), may hold values from -0.125 to 0.125
- w_conv_right: bfloat16 [2048, 2048], P(None, 'tp'), may hold values from -0.125 to 0.125
- conv_taps: float32 [3, 2048], replicated, may hold values from -3.5 to 3.5
- first_memory: float32 [8, 128, 256], P('tp'), may hold values from -2560 to 2560
- first_norm: float32 [8, 128], P('tp'), may hold values from -2560 to 2560
- w_out_memory: bfloat16 [2048, 2048], P('tp'), may hold values from -0.09375 to 0.09375
- w_out_conv: bfloat16 [2048, 2048], P('tp'), may hold values from -0.09375 to 0.09375
Outputs:
- mixed: bfloat16 [6144, 2048], P(('sp', 'tp'))
The draws below stay inside these ranges and needn't reach their ends.
All inputs are finite; a program needn't handle non-finite values.
Results may differ from the reference program's by a relative error of at most 0.015.
The reference program's roundings to bfloat16 on the way count: a program that leaves them out, or rounds other values in their place, can miss the bound.
Values may be sent and summed in bfloat16 or wider, within the bound.
No kernel may reach another device: no remote copies, remote signals or barrier semaphores. Data moves between devices by JAX's collectives and lax.ppermute only.
A program may use at most 64 MiB of HBM per device.

```python
import math
import jax
import jax.numpy as jnp
from jax import lax

D = 2048
MEMORY_HEADS = 8
KEY_DIM = 128
VALUE_DIM = 256
CONV_CH = 2048
TAPS = 3
TOK_DEV = 768
SEQUENCE_TOKENS = 6144
QK_WIDTH = 1024
V_WIDTH = 2048
N_TP = 4


def decay_plan(key):
    base_key = jax.random.fold_in(key, 7)
    order_key, spread_key, block_key, place_key, loss_key = jax.random.split(base_key, 5)
    fast_heads = jax.random.permutation(order_key, MEMORY_HEADS) < MEMORY_HEADS // 2
    spread = jax.random.uniform(spread_key, (MEMORY_HEADS,), jnp.float32)
    head_bias = jnp.where(fast_heads, 4.0 + 1.5 * spread, math.log(SEQUENCE_TOKENS) + 1.5 + spread)
    return (head_bias, block_key, place_key, loss_key)


def draw_forget_bias(key, part):
    head_bias, block_key, place_key, loss_key = decay_plan(key)
    return head_bias.astype(jnp.float32)


def draw_forget_extra(key, part):
    head_bias, block_key, place_key, loss_key = decay_plan(key)
    head_rate = jnp.exp(-head_bias)
    factor = jax.random.uniform(block_key, (SEQUENCE_TOKENS // TOK_DEV, MEMORY_HEADS), jnp.float32, 0.0, 2.0)
    block_portion = -jnp.repeat(factor, TOK_DEV, axis=0) * head_rate[None, :]
    place_slots = jax.random.randint(place_key, (3, MEMORY_HEADS), 0, SEQUENCE_TOKENS)
    loss_values = jnp.log(jax.random.uniform(loss_key, (3, MEMORY_HEADS), jnp.float32, 0.6, 0.8))
    token_positions = jnp.arange(SEQUENCE_TOKENS, dtype=jnp.int32)
    span_total_sum = jnp.zeros((SEQUENCE_TOKENS, MEMORY_HEADS), jnp.float32)
    for token_span in range(3):
        span_total_sum = span_total_sum + jnp.where(token_positions[:, None] == place_slots[token_span][None, :], loss_values[token_span][None, :], 0.0)
    return (block_portion + span_total_sum).astype(jnp.float32)


def draw_w_input_gate(key, part):
    weights = jax.random.normal(jax.random.fold_in(key, 11), (D, MEMORY_HEADS), jnp.float32) / math.sqrt(D)
    return jnp.clip(weights, -8.0, 8.0).astype(jnp.bfloat16)


def steps_of(key, extent, cuts, least, top_value):
    loudness, own = 1.0, jax.random.fold_in(key, 6)
    for position, blocks in cuts:
        heights = jnp.exp(jax.random.uniform(jax.random.fold_in(own, position), (blocks,), jnp.float32, least / len(cuts), top_value / len(cuts)))
        loudness = loudness * jnp.repeat(heights, extent[position] // blocks).reshape([-1 if axis == position else 1 for axis in range(len(extent))])
    return loudness


def noise(own_key, shape, scale, bound, pieces=(), held_as=jnp.bfloat16):
    drawn = jax.random.normal(own_key, shape, jnp.float32) * scale
    if len(pieces) > 0:
        drawn = steps_of(own_key, shape, pieces, -0.22, 0.18) * drawn
    return jnp.clip(drawn, min=-bound, max=bound).astype(held_as)


def setup_inputs(seed: int = 0) -> dict:
    splits = jax.random.split(jax.random.key(seed), 18)
    return {
        "tokens": noise(splits[0], (SEQUENCE_TOKENS, D), 1.0, 6.0, ((0, 32),)),
        "in_gain": jnp.clip(1.0 + 0.18 * jax.random.normal(splits[1], (D,), jnp.float32), 0.1, 1.9),
        "w_query": noise(splits[2], (D, QK_WIDTH), D ** -0.5, 0.125, ((1, 4),)),
        "w_key": noise(splits[3], (D, QK_WIDTH), D ** -0.5, 0.125, ((1, 4),)),
        "w_value": noise(splits[4], (D, V_WIDTH), D ** -0.5, 0.125, ((1, 4),)),
        "w_input_gate": draw_w_input_gate(jax.random.fold_in(splits[17], 71), 0),
        "w_forget_gate": noise(splits[6], (D, MEMORY_HEADS), D ** -0.5, 0.125),
        "forget_bias": draw_forget_bias(jax.random.fold_in(splits[17], 71), 0),
        "forget_extra": draw_forget_extra(jax.random.fold_in(splits[17], 71), 0),
        "w_conv_gate": noise(splits[9], (D, CONV_CH), D ** -0.5, 0.125, ((1, 4),)),
        "w_conv_left": noise(splits[10], (D, CONV_CH), D ** -0.5, 0.125, ((1, 4),)),
        "w_conv_right": noise(splits[11], (D, CONV_CH), D ** -0.5, 0.125, ((1, 4),)),
        "conv_taps": noise(splits[12], (TAPS, CONV_CH), TAPS ** -0.5, 3.5, (), jnp.float32),
        "first_memory": noise(splits[13], (MEMORY_HEADS, KEY_DIM, VALUE_DIM), (6 * SEQUENCE_TOKENS ** 0.5), 2560.0, ((0, 4),), jnp.float32),
        "first_norm": noise(splits[14], (MEMORY_HEADS, KEY_DIM), (6 * SEQUENCE_TOKENS ** 0.5), 2560.0, ((0, 4),), jnp.float32),
        "w_out_memory": noise(splits[15], (V_WIDTH, D), (V_WIDTH + CONV_CH) ** -0.5, 0.09375, ((0, 4),)),
        "w_out_conv": noise(splits[16], (CONV_CH, D), (V_WIDTH + CONV_CH) ** -0.5, 0.09375, ((0, 4),)),
    }


epsilon = 1e-06

def rounded(values):
    return lax.optimization_barrier(values.astype(jnp.bfloat16)).astype(jnp.float32)

def mixer_block(carried_state, inputs):
    carry_max, carry_memory, carry_norm = carried_state
    query_rows, key_rows, value_rows, in_pre, log_forget = inputs
    length = query_rows.shape[0]
    query_scale = KEY_DIM ** (-0.5)
    cumulative = jnp.cumsum(log_forget, axis=0)
    decay_total = cumulative[length - 1]
    weight_log = decay_total[None, :] - cumulative + in_pre
    block_max = lax.optimization_barrier(jnp.max(weight_log, axis=0))
    keyed = key_rows.astype(jnp.float32) * jnp.exp(weight_log - block_max[None, :])[:, :, None]
    block_norm = lax.optimization_barrier(jnp.sum(keyed, axis=0))
    block_memory = jnp.einsum('shd,shv->hdv', rounded(keyed), value_rows.astype(jnp.float32))
    token_positions = jnp.arange(length, dtype=jnp.int32)
    causal = token_positions[:, None] >= token_positions[None, :]
    cum_heads = cumulative.T
    log_gap = cum_heads[:, :, None] - cum_heads[:, None, :] + in_pre.T[:, None, :]
    log_gap = jnp.where(causal[None], log_gap, -jnp.inf)
    inter_log = cum_heads + carry_max[:, None]
    row_max = jnp.maximum(inter_log, lax.optimization_barrier(jnp.max(log_gap, axis=2)))
    raw_scores = jnp.einsum('thd,shd->hts', query_rows.astype(jnp.float32), key_rows.astype(jnp.float32)) * query_scale
    mixing = raw_scores * jnp.exp(log_gap - row_max[:, :, None])
    carried = jnp.exp(inter_log - row_max).T
    scaled_query = query_rows.astype(jnp.float32) * query_scale
    from_values = jnp.einsum('hts,shv->thv', rounded(mixing), value_rows.astype(jnp.float32))
    from_memory = jnp.einsum('thd,hdv->thv', scaled_query, carry_memory, precision=lax.Precision.HIGHEST)
    from_norm = jnp.einsum('thd,hd->th', scaled_query, carry_norm, precision=lax.Precision.HIGHEST)
    numerator = from_values + carried[:, :, None] * from_memory
    denominator = lax.optimization_barrier(jnp.sum(mixing, axis=2)).T + carried * from_norm
    memory_out = numerator / jnp.maximum(jnp.abs(denominator), 1.0)[:, :, None]
    row_mean = lax.optimization_barrier(jnp.mean(memory_out * memory_out, axis=(1, 2), keepdims=True))
    heads_out = (memory_out * lax.rsqrt(row_mean + epsilon)).astype(jnp.bfloat16)
    new_max = jnp.maximum(carry_max + decay_total, block_max)
    old_scale = jnp.exp(carry_max + decay_total - new_max)
    new_scale = jnp.exp(block_max - new_max)
    new_memory = old_scale[:, None, None] * carry_memory + new_scale[:, None, None] * block_memory
    new_norm = old_scale[:, None] * carry_norm + new_scale[:, None] * block_norm
    return ((new_max, new_memory, new_norm), heads_out)

def reference(tokens, in_gain, w_query, w_key, w_value, w_input_gate, w_forget_gate, forget_bias, forget_extra, w_conv_gate, w_conv_left, w_conv_right, conv_taps, first_memory, first_norm, w_out_memory, w_out_conv):
    token_rows = tokens.astype(jnp.float32)
    scale_rows = lax.rsqrt(lax.optimization_barrier(jnp.mean(token_rows * token_rows, axis=1, keepdims=True)) + epsilon)
    normed = (token_rows * scale_rows * in_gain).astype(jnp.bfloat16)
    query_rows = jnp.dot(normed, w_query, preferred_element_type=jnp.float32).astype(jnp.bfloat16)
    key_rows = jnp.dot(normed, w_key, preferred_element_type=jnp.float32).astype(jnp.bfloat16)
    value_rows = jnp.dot(normed, w_value, preferred_element_type=jnp.float32).astype(jnp.bfloat16)
    in_pre = jnp.dot(normed, w_input_gate, preferred_element_type=jnp.float32)
    forget_pre = jnp.dot(normed, w_forget_gate, preferred_element_type=jnp.float32) + forget_bias
    log_forget = jax.nn.log_sigmoid(forget_pre) + forget_extra
    conv_gate = rounded(jnp.dot(normed, w_conv_gate, preferred_element_type=jnp.float32))
    conv_left = rounded(jnp.dot(normed, w_conv_left, preferred_element_type=jnp.float32))
    conv_right = rounded(jnp.dot(normed, w_conv_right, preferred_element_type=jnp.float32))
    product = (conv_left * conv_right).astype(jnp.bfloat16)
    padded = jnp.concatenate([jnp.zeros((TAPS - 1, CONV_CH), jnp.bfloat16), product], axis=0).astype(jnp.float32)
    filtered = conv_taps[0][None, :] * padded[0:SEQUENCE_TOKENS]
    for tap_index in range(1, TAPS):
        filtered = filtered + conv_taps[tap_index][None, :] * padded[tap_index:tap_index + SEQUENCE_TOKENS]
    conv_branch = (conv_gate * filtered).astype(jnp.bfloat16)
    blocks = SEQUENCE_TOKENS // TOK_DEV
    inputs = (query_rows.reshape(blocks, TOK_DEV, MEMORY_HEADS, KEY_DIM), key_rows.reshape(blocks, TOK_DEV, MEMORY_HEADS, KEY_DIM), value_rows.reshape(blocks, TOK_DEV, MEMORY_HEADS, VALUE_DIM), in_pre.reshape(blocks, TOK_DEV, MEMORY_HEADS), log_forget.reshape(blocks, TOK_DEV, MEMORY_HEADS))
    start_state = (jnp.zeros((MEMORY_HEADS,), jnp.float32), first_memory, first_norm)
    final_state, heads_out = lax.scan(mixer_block, start_state, inputs)
    heads_out = heads_out.reshape(SEQUENCE_TOKENS, V_WIDTH)
    head_group = V_WIDTH // N_TP
    channel_group = CONV_CH // N_TP
    mixed = jnp.zeros((SEQUENCE_TOKENS, D), jnp.float32)
    for group in range(N_TP):
        head_lo = group * head_group
        channel_lo = group * channel_group
        partial_value = jnp.dot(heads_out[:, head_lo:head_lo + head_group], w_out_memory[head_lo:head_lo + head_group], preferred_element_type=jnp.float32)
        partial_value = partial_value + jnp.dot(conv_branch[:, channel_lo:channel_lo + channel_group], w_out_conv[channel_lo:channel_lo + channel_group], preferred_element_type=jnp.float32)
        mixed = mixed + rounded(partial_value)
    return mixed.astype(jnp.bfloat16)
```

```python
import jax
import jax.numpy as jnp
from jax import lax
from jax.experimental import pallas as pl
from jax.experimental.pallas import tpu as pltpu
from jax.sharding import PartitionSpec as P


KEY_DIM = 128
VALUE_DIM = 256
TAPS = 3
CORES = 2
LANES = 128
EDGE = 16
EPSILON = 1e-06
VERY_NEGATIVE = -1e30
QUERY_SCALE = KEY_DIM ** (-0.5)
F32 = jnp.float32
BF16 = jnp.bfloat16


def dot(a, b):
    return jnp.dot(a, b, preferred_element_type=F32)


def shape(rows, columns, dtype):
    return jax.ShapeDtypeStruct((rows, columns), dtype)


def run(body, outs, *args, scalars=0, scratch=(), flops=0, limit=16):
    in_specs = [pl.BlockSpec(memory_space=pltpu.SMEM)] * scalars
    in_specs += [pl.BlockSpec(memory_space=pltpu.VMEM)] * (len(args) - scalars)
    args = [
        a if i < scalars else pltpu.with_memory_space_constraint(a, pltpu.VMEM)
        for i, a in enumerate(args)
    ]
    return pl.pallas_call(
        body,
        out_shape=[pltpu.VMEM(o.shape, o.dtype) for o in outs],
        in_specs=in_specs,
        out_specs=[pl.BlockSpec(memory_space=pltpu.VMEM)] * len(outs),
        scratch_shapes=scratch,
        cost_estimate=pl.CostEstimate(flops=flops, bytes_accessed=0, transcendentals=0),
        compiler_params=pltpu.CompilerParams(vmem_limit_bytes=limit << 20),
    )(*args)


def xor(block, axis, distance):
    return lax.ppermute(block, axis, [(i, i ^ distance) for i in range(lax.axis_size(axis))])


def place(tp, piece, rows):
    return pl.ds(pl.multiple_of(jnp.bitwise_xor(tp, piece) * rows, rows), rows)


def normalize(tokens, gain):
    wide = tokens.astype(F32)
    scale = lax.rsqrt(jnp.mean(wide * wide, axis=1, keepdims=True) + EPSILON)
    return (wide * scale * gain).astype(BF16)


def project_kv(blocks, gain, w_key, w_value, w_gates, normed, kv, gates):
    rows = blocks[0].shape[0]
    width = w_key.shape[1]
    for i, block in enumerate(blocks):
        normed[i * rows : (i + 1) * rows] = normalize(block[...], gain[...])
    gates[...] = dot(normed[...], w_gates[...])
    kv[:, :width] = dot(normed[...], w_key[...]).astype(BF16)
    kv[:, width:] = dot(normed[...], w_value[...]).astype(BF16)


def kv_kernel(*refs):
    project_kv(refs[:-7], *refs[-7:])


def pieces3(x):
    high = x.astype(BF16).astype(F32)
    rest = x - high
    middle = rest.astype(BF16).astype(F32)
    return high, middle, rest - middle


def write_payload(payload, memory, small):
    width = memory.shape[0]
    payload[:width] = memory.astype(BF16)
    high, middle, low = pieces3(small)
    extra = jnp.concatenate(
        [
            jnp.concatenate([high, middle], axis=1),
            jnp.concatenate([low, jnp.zeros_like(low)], axis=1),
        ],
        axis=0,
    )
    payload[width:] = extra.astype(BF16)


def read_payload(payload):
    width = payload.shape[0] - 16
    extra = payload[width:].astype(F32)
    small = extra[:8, :LANES] + extra[:8, LANES:] + extra[8:, :LANES]
    return payload[:width].astype(F32), small


def state_kernel(n_blocks, n_a, n_b, *refs):
    tp_ref, refs = refs[0], refs[1:]
    blocks, refs = refs[:n_blocks], refs[n_blocks:]
    gain, w_key, w_value, w_gates, kv_a, kv_b, gates_a, gates_b, extra, bias = refs[:10]
    normed, kv_all, score_log, memory, small, payload = refs[10:16]
    kv_c, gates_c, gates_all = refs[16:]
    project_kv(blocks, gain, w_key, w_value, w_gates, normed, kv_c, gates_c)
    tp = tp_ref[0]
    rows = blocks[0].shape[0]
    sources = [(i, kv_a, gates_a, i) for i in range(n_a)]
    sources += [(CORES * (i + 1), kv_b, gates_b, i) for i in range(n_b)]
    sources += [(CORES * (i + 1) + 1, kv_c, gates_c, i) for i in range(n_blocks)]
    for piece, kv, gates, at in sources:
        kv_all[place(tp, piece, rows)] = kv[at * rows : (at + 1) * rows]
        gates_all[place(tp, piece, rows)] = gates[at * rows : (at + 1) * rows]
    length = kv_all.shape[0]
    width = w_key.shape[1]
    heads = width // KEY_DIM
    forget = gates_all[:, LANES:] + bias[...]
    log_forget = jnp.minimum(forget, 0.0) - jnp.log1p(jnp.exp(-jnp.abs(forget))) + extra[...]
    row = lax.broadcasted_iota(jnp.int32, (length, length), 0)
    column = lax.broadcasted_iota(jnp.int32, (length, length), 1)
    ones = jnp.where(row >= column, 1.0, 0.0).astype(BF16)
    high, middle, low = pieces3(log_forget)
    cumulative = dot(ones, high.astype(BF16)) + (
        dot(ones, middle.astype(BF16)) + dot(ones, low.astype(BF16))
    )
    score = gates_all[:, :LANES] - cumulative
    score_log[...] = score
    decay = cumulative[length - 1 : length]
    weight_log = decay + score
    block_max = jnp.max(weight_log, axis=0, keepdims=True)
    weight = jnp.exp(weight_log - block_max)
    small[...] = jnp.zeros_like(small)
    small[0:1] = decay
    small[1:2] = block_max
    for h in range(heads):
        keys = slice(h * KEY_DIM, (h + 1) * KEY_DIM)
        values = slice(width + h * VALUE_DIM, width + (h + 1) * VALUE_DIM)
        keyed = kv_all[:, keys].astype(F32) * weight[:, h : h + 1]
        small[2 + h : 3 + h] = jnp.sum(keyed, axis=0, keepdims=True)
        memory[keys] = lax.dot_general(
            keyed.astype(BF16),
            kv_all[:, values],
            (((0,), (0,)), ((), ())),
            preferred_element_type=F32,
        )
    write_payload(payload, memory[...], small[...])


def rest_kernel(normed, w_query, w_gate, w_left, w_right, query, gate, product):
    query[...] = dot(normed[...], w_query[...]).astype(BF16)
    gate[...] = dot(normed[...], w_gate[...]).astype(BF16)
    left = dot(normed[...], w_left[...]).astype(BF16).astype(F32)
    right = dot(normed[...], w_right[...]).astype(BF16).astype(F32)
    product[...] = (left * right).astype(BF16)


def conv_kernel(n_a, n_b, n_c, *refs):
    tp_ref, normed_b, normed_c, edge, gain = refs[:5]
    w_query, w_gate, w_left, w_right, taps, query_a, gate_a, product_a = refs[5:13]
    query_all, branch = refs[13:15]
    normed, gate_all, padded = refs[15:]
    tp = tp_ref[0]
    n = n_b + n_c
    rows = normed_b.shape[0] // n_b
    length = query_all.shape[0]
    normed[: n_b * rows] = normed_b[...]
    normed[n_b * rows : n * rows] = normed_c[...]
    normed[n * rows :] = normalize(edge[...], gain[...])
    order = [CORES * (i + 1) for i in range(n_b)] + [CORES * (i + 1) + 1 for i in range(n_c)]
    query = dot(normed[: n * rows], w_query[...]).astype(BF16)
    gate = dot(normed[: n * rows], w_gate[...])
    left = dot(normed[...], w_left[...]).astype(BF16).astype(F32)
    right = dot(normed[...], w_right[...]).astype(BF16).astype(F32)
    product = (left * right).astype(BF16).astype(F32)
    padded[:EDGE] = product[n * rows :]
    for at, piece in enumerate(order):
        here = slice(at * rows, (at + 1) * rows)
        query_all[place(tp, piece, rows)] = query[here]
        gate_all[place(tp, piece, rows)] = gate[here].astype(BF16)
        start = pl.multiple_of(jnp.bitwise_xor(tp, piece) * rows + EDGE, EDGE)
        padded[pl.ds(start, rows)] = product[here]
    for piece in range(n_a):
        here = slice(piece * rows, (piece + 1) * rows)
        query_all[place(tp, piece, rows)] = query_a[here]
        gate_all[place(tp, piece, rows)] = gate_a[here]
        start = pl.multiple_of(jnp.bitwise_xor(tp, piece) * rows + EDGE, EDGE)
        padded[pl.ds(start, rows)] = product_a[here].astype(F32)
    first = EDGE - (TAPS - 1)
    filtered = taps[0:1] * padded[first : first + length]
    for tap in range(1, TAPS):
        filtered = filtered + taps[tap : tap + 1] * padded[first + tap : first + tap + length]
    branch[...] = (gate_all[...].astype(F32) * filtered).astype(BF16)


def inner_kernel(query, kv, score_log, from_values, row_log, row_sum):
    length, width = query.shape
    heads = width // KEY_DIM
    score_rows = score_log[...].T
    step = 256
    lane = lax.broadcasted_iota(jnp.int32, (step, LANES), 1)
    for first in range(0, length, step):
        last = first + step
        here = slice(first, last)
        logs = jnp.zeros((step, LANES), F32)
        sums = jnp.zeros((step, LANES), F32)
        row = lax.broadcasted_iota(jnp.int32, (step, last), 0) + first
        column = lax.broadcasted_iota(jnp.int32, (step, last), 1)
        for h in range(heads):
            keys = slice(h * KEY_DIM, (h + 1) * KEY_DIM)
            values = slice(width + h * VALUE_DIM, width + (h + 1) * VALUE_DIM)
            raw = lax.dot_general(
                query[here, keys],
                kv[:last, keys],
                (((1,), (1,)), ((), ())),
                preferred_element_type=F32,
            )
            log = jnp.where(row >= column, score_rows[h : h + 1, :last], VERY_NEGATIVE)
            top = jnp.max(log, axis=1, keepdims=True)
            mixing = raw * QUERY_SCALE * jnp.exp(log - top)
            logs = jnp.where(lane == h, top, logs)
            sums = jnp.where(lane == h, jnp.sum(mixing, axis=1, keepdims=True), sums)
            from_values[here, h * VALUE_DIM : (h + 1) * VALUE_DIM] = dot(
                mixing.astype(BF16), kv[:last, values]
            )
        row_log[here] = logs
        row_sum[here] = sums


def scales(early, late):
    top = jnp.maximum(early[1:2] + late[0:1], late[1:2])
    return top, jnp.exp(early[1:2] + late[0:1] - top), jnp.exp(late[1:2] - top)


def join(early_memory, early, late_memory, late, memory, small):
    top, scale_early, scale_late = scales(early, late)
    small[0:1] = early[0:1] + late[0:1]
    small[1:2] = top
    for h in range(memory.shape[0] // KEY_DIM):
        keys = slice(h * KEY_DIM, (h + 1) * KEY_DIM)
        a, b = scale_early[:, h : h + 1], scale_late[:, h : h + 1]
        memory[keys] = a * early_memory[keys] + b * late_memory[keys]
        small[2 + h : 3 + h] = a * early[2 + h : 3 + h] + b * late[2 + h : 3 + h]


def empty(small):
    row = lax.broadcasted_iota(jnp.int32, small.shape, 0)
    return jnp.where(row == 1, VERY_NEGATIVE, 0.0)


def join_kernel(distance, has_prior, *refs):
    sp_ref, total_memory, total_small, received = refs[:4]
    refs = refs[4:]
    if has_prior:
        prior_memory, prior_small = refs[:2]
        refs = refs[2:]
    new_memory, new_small, next_memory, next_small, payload = refs
    late = jnp.bitwise_and(sp_ref[0], distance) != 0
    their_memory, their_small = read_payload(received)

    new_small[...] = jnp.zeros_like(new_small)
    next_small[...] = jnp.zeros_like(next_small)

    @pl.when(late)
    def _():
        join(their_memory, their_small, total_memory, total_small, new_memory, new_small)
        if has_prior:
            join(their_memory, their_small, prior_memory, prior_small, next_memory, next_small)
        else:
            next_memory[...] = their_memory
            next_small[...] = their_small

    @pl.when(jnp.logical_not(late))
    def _():
        join(total_memory, total_small, their_memory, their_small, new_memory, new_small)
        if has_prior:
            next_memory[...] = prior_memory[...]
            next_small[...] = prior_small[...]
        else:
            next_memory[...] = jnp.zeros_like(next_memory)
            next_small[...] = empty(next_small)

    write_payload(payload, new_memory[...], new_small[...])


def memory_kernel(distance, *refs):
    sp_ref, prior_memory, prior_small, received, first_memory, first_norm = refs[:6]
    query, from_values, row_log, row_sum, out, squares = refs[6:12]
    enter_memory, enter_small = refs[12:]
    heads = prior_memory.shape[0] // KEY_DIM
    late = jnp.bitwise_and(sp_ref[0], distance) != 0
    enter_small[...] = jnp.zeros_like(enter_small)

    @pl.when(late)
    def _():
        their_memory, their_small = read_payload(received)
        join(their_memory, their_small, prior_memory, prior_small, enter_memory, enter_small)

    @pl.when(jnp.logical_not(late))
    def _():
        enter_memory[...] = prior_memory[...]
        enter_small[...] = prior_small[...]

    decay, top = enter_small[0:1], enter_small[1:2]
    enter_max = jnp.maximum(top, decay)
    from_prior = jnp.exp(top - enter_max)
    from_first = jnp.exp(decay - enter_max)
    length = query.shape[0]
    total = jnp.zeros((length, 1), F32)
    for h in range(heads):
        keys = slice(h * KEY_DIM, (h + 1) * KEY_DIM)
        values = slice(h * VALUE_DIM, (h + 1) * VALUE_DIM)
        a, b = from_prior[:, h : h + 1], from_first[:, h : h + 1]
        carry_memory = a * enter_memory[keys] + b * first_memory[keys]
        carry_norm = a * enter_small[2 + h : 3 + h] + b * first_norm[h : h + 1]
        high = carry_memory.astype(BF16)
        low = (carry_memory - high.astype(F32)).astype(BF16)
        rows = query[:, keys]
        by_norm = jnp.sum(rows.astype(F32) * carry_norm, axis=1, keepdims=True)
        inner_log = row_log[:, h : h + 1]
        carry_max = enter_max[:, h : h + 1]
        row_max = jnp.maximum(inner_log, carry_max)
        inner = jnp.exp(inner_log - row_max)
        outer = jnp.exp(carry_max - row_max) * QUERY_SCALE
        below = inner * row_sum[:, h : h + 1] + outer * by_norm
        over = 1.0 / jnp.maximum(jnp.abs(below), 1.0)
        by_memory = dot(rows, high) + dot(rows, low)
        result = (inner * over) * from_values[:, values] + (outer * over) * by_memory
        total = total + jnp.sum(result * result, axis=1, keepdims=True)
        out[:, values] = result.astype(BF16)
    squares[...] = jnp.broadcast_to(total, (length, LANES)).T[:8]


def out_kernel(pieces, all_values, *refs):
    tp_ref, memory_out, branch, squares, w_memory, w_conv, keep, send, scale = refs
    tp = tp_ref[0]
    rows = keep.shape[0] * CORES // len(pieces)
    length, width = memory_out.shape[0], keep.shape[1]
    total = jnp.broadcast_to(squares[0:1], (LANES, length)).T
    scale[...] = lax.rsqrt(total / all_values + EPSILON)
    step = 512
    for i, piece in enumerate(pieces):
        here = place(tp, piece, rows)
        to = send if piece % CORES else keep
        at = slice((i // CORES) * rows, (i // CORES + 1) * rows)
        heads = memory_out[here]
        conv = branch[here]
        by = scale[here, 0:1]
        for first in range(0, width, step):
            columns = slice(first, first + step)
            part = by * dot(heads, w_memory[:, columns]) + dot(conv, w_conv[:, columns])
            to[at, columns] = part.astype(BF16)


def per_device(
    tokens,
    in_gain,
    w_query,
    w_key,
    w_value,
    w_input_gate,
    w_forget_gate,
    forget_bias,
    forget_extra,
    w_conv_gate,
    w_conv_left,
    w_conv_right,
    conv_taps,
    first_memory,
    first_norm,
    w_out_memory,
    w_out_conv,
):
    n_tp, n_sp = lax.axis_size("tp"), lax.axis_size("sp")
    n_y = n_tp // CORES
    rows, depth = tokens.shape
    length = rows * n_tp
    width = w_query.shape[1]
    value_width = w_value.shape[1]
    heads = width // KEY_DIM
    channels = w_conv_gate.shape[1]
    tp, sp = lax.axis_index("tp"), lax.axis_index("sp")
    tp_at, sp_at = tp.reshape(1), sp.reshape(1)

    direct = [xor(tokens, "tp", CORES * i) for i in range(1, n_y)]
    partner = xor(tokens, "tp", 1)
    passed = [xor(block, "tp", 1) for block in direct]

    last = n_tp - 1
    edge = lax.ppermute(
        tokens[rows - EDGE :],
        ("sp", "tp"),
        [(s * n_tp + last, (s + 1) * n_tp + last) for s in range(n_sp - 1)],
    )
    edge = edge + lax.ppermute(edge, "tp", [(last, last - 1)])
    ends = [last, last - 1]
    edge_far = [lax.ppermute(edge, "tp", [(a, a - CORES * i) for a in ends]) for i in range(1, n_y)]
    for block in edge_far:
        edge = edge + block

    head_first = tp * heads
    gate_columns = [
        lax.dynamic_slice_in_dim(w, head_first, heads, 1) for w in (w_input_gate, w_forget_gate)
    ]
    pad = ((0, 0), (0, LANES - heads))
    w_gates = jnp.concatenate([jnp.pad(w, pad) for w in gate_columns], axis=1)
    bias = jnp.pad(lax.dynamic_slice_in_dim(forget_bias, head_first, heads, 0)[None], pad)
    extra = jnp.pad(forget_extra, pad)
    gain = in_gain[None]
    taps = lax.dynamic_slice_in_dim(conv_taps, tp * channels, channels, 1)

    def kv_of(blocks):
        n = len(blocks) * rows
        return run(
            kv_kernel,
            [shape(n, depth, BF16), shape(n, width + value_width, BF16), shape(n, 2 * LANES, F32)],
            *blocks,
            gain,
            w_key,
            w_value,
            w_gates,
            flops=2 * n * depth * (width + value_width),
        )

    normed_a, kv_a, gates_a = kv_of([tokens, partner])
    n_a = CORES * rows
    query_a, gate_a, product_a = run(
        rest_kernel,
        [shape(n_a, width, BF16), shape(n_a, channels, BF16), shape(n_a, channels, BF16)],
        normed_a,
        w_query,
        w_conv_gate,
        w_conv_left,
        w_conv_right,
        flops=2 * n_a * depth * (width + 3 * channels),
    )
    normed_b, kv_b, gates_b = kv_of(direct)
    n_c = len(passed) * rows
    normed_c, kv_all, score_log, memory, small, payload = run(
        lambda *refs: state_kernel(len(passed), CORES, len(direct), *refs),
        [
            shape(n_c, depth, BF16),
            shape(length, width + value_width, BF16),
            shape(length, LANES, F32),
            shape(width, VALUE_DIM, F32),
            shape(8, LANES, F32),
            shape(width + 16, VALUE_DIM, BF16),
        ],
        tp_at,
        *passed,
        gain,
        w_key,
        w_value,
        w_gates,
        kv_a,
        kv_b,
        gates_a,
        gates_b,
        extra,
        bias,
        scalars=1,
        scratch=[
            pltpu.VMEM((n_c, width + value_width), BF16),
            pltpu.VMEM((n_c, 2 * LANES), F32),
            pltpu.VMEM((length, 2 * LANES), F32),
        ],
        flops=2 * n_c * depth * (width + value_width),
    )
    n_bc = len(direct + passed) * rows
    query_all, branch = run(
        lambda *refs: conv_kernel(CORES, len(direct), len(passed), *refs),
        [shape(length, width, BF16), shape(length, channels, BF16)],
        tp_at,
        normed_b,
        normed_c,
        edge,
        gain,
        w_query,
        w_conv_gate,
        w_conv_left,
        w_conv_right,
        taps,
        query_a,
        gate_a,
        product_a,
        scalars=1,
        scratch=[
            pltpu.VMEM((n_bc + EDGE, depth), BF16),
            pltpu.VMEM((length, channels), BF16),
            pltpu.VMEM((length + EDGE, channels), F32),
        ],
        flops=2 * n_bc * depth * (width + 3 * channels),
    )
    from_values, row_log, row_sum = run(
        inner_kernel,
        [shape(length, value_width, F32), shape(length, LANES, F32), shape(length, LANES, F32)],
        query_all,
        kv_all,
        score_log,
        flops=2 * heads * length * length * (KEY_DIM + VALUE_DIM),
    )

    prior = ()
    distance = 1
    while distance < n_sp // 2:
        received = xor(payload, "sp", distance)
        memory, small, next_memory, next_small, payload = run(
            lambda *refs, d=distance, p=len(prior) > 0: join_kernel(d, p, *refs),
            [shape(width, VALUE_DIM, F32), shape(8, LANES, F32)] * 2
            + [shape(width + 16, VALUE_DIM, BF16)],
            sp_at,
            memory,
            small,
            received,
            *prior,
            scalars=1,
            flops=8 * width * VALUE_DIM,
        )
        prior = (next_memory, next_small)
        distance *= 2
    received = xor(payload, "sp", distance)
    memory_out, squares = run(
        lambda *refs: memory_kernel(distance, *refs),
        [shape(length, value_width, BF16), shape(8, length, F32)],
        sp_at,
        *prior,
        received,
        first_memory.reshape(width, VALUE_DIM),
        first_norm,
        query_all,
        from_values,
        row_log,
        row_sum,
        scalars=1,
        scratch=[pltpu.VMEM((width, VALUE_DIM), F32), pltpu.VMEM((8, LANES), F32)],
        flops=4 * length * width * VALUE_DIM,
    )

    squares = squares + xor(squares, "tp", 1)
    far = [xor(squares, "tp", CORES * i) for i in range(1, n_y)]
    for block in far:
        squares = squares + block

    def projected(pieces):
        n = len(pieces) // CORES * rows
        return run(
            lambda *refs: out_kernel(pieces, value_width * n_tp, *refs),
            [shape(n, depth, BF16), shape(n, depth, BF16)],
            tp_at,
            memory_out,
            branch,
            squares,
            w_out_memory,
            w_out_conv,
            scalars=1,
            scratch=[pltpu.VMEM((length, LANES), F32)],
            flops=2 * CORES * n * depth * (value_width + channels),
        )

    keep_far, send_far = projected(list(range(CORES, n_tp)))
    pair_far = (keep_far.astype(F32) + xor(send_far, "tp", 1).astype(F32)).astype(BF16)
    arrived = [xor(pair_far[(i - 1) * rows : i * rows], "tp", CORES * i) for i in range(1, n_y)]
    keep_own, send_own = projected(list(range(CORES)))
    mixed = keep_own.astype(F32) + xor(send_own, "tp", 1).astype(F32)
    for block in arrived:
        mixed = mixed + block.astype(F32)
    return mixed.astype(BF16)


def solution(mesh):
    in_specs = (
        P(("sp", "tp"), None),
        P(),
        P(None, "tp"),
        P(None, "tp"),
        P(None, "tp"),
        P(),
        P(),
        P(),
        P("sp", "tp"),
        P(None, "tp"),
        P(None, "tp"),
        P(None, "tp"),
        P(),
        P("tp", None, None),
        P("tp", None),
        P("tp", None),
        P("tp", None),
    )
    out_specs = P(("sp", "tp"), None)
    return jax.shard_map(
        per_device, mesh=mesh, in_specs=in_specs, out_specs=out_specs, check_vma=False
    )
```
